32 devices in a mesh: sp: 16 (over z, y, core), fs: 1, tp: 2 (over x).
Axes of the slice: x: 2, y: 2, z: 4, core: 2. Of those that a mesh axis runs over, the one named last changes fastest.
Arguments:
- tokens: bfloat16 [1, 4096, 2048], P('fs', 'sp'), may hold values from -6 to 6
- norm_gain: float32 [2048], replicated, may hold values from 0.1 to 1.9
- w_state_in: bfloat16 [2048, 1024], P(('sp', 'fs'), 'tp'), may hold values from -0.125 to 0.125
- w_value: bfloat16 [2048, 1024], P(('sp', 'fs'), 'tp'), may hold values from -0.125 to 0.125
- w_outer: bfloat16 [2048, 1024], P(('sp', 'fs'), 'tp'), may hold values from -0.125 to 0.125
- w_inner: bfloat16 [2048, 1024], P(('sp', 'fs'), 'tp'), may hold values from -0.125 to 0.125
- w_state_out: bfloat16 [2048, 1024], P(('sp', 'fs'), 'tp'), may hold values from -0.125 to 0.125
- w_conv_out: bfloat16 [2048, 1024], P(('sp', 'fs'), 'tp'), may hold values from -0.125 to 0.125
- log_step: float32 [64], P('tp'), may hold values from -4.6 to -3.2
- decay_real: float32 [64, 64], P('tp'), may hold values from -5 to 0
- frequency: float32 [64, 64], P('tp'), may hold values from 1 to 192
- step_rate: float32 [1, 4096], P('fs', 'sp'), may hold values from 0.4 to 2.5
- input_real: float32 [64, 64, 16], P('tp'), may hold values from -1 to 1
- input_imag: float32 [64, 64, 16], P('tp'), may hold values from -1 to 1
- read_real: float32 [64, 16, 64], P('tp'), may hold values from -0.75 to 0.75
- read_imag: float32 [64, 16, 64], P('tp'), may hold values from -0.75 to 0.75
- skip_gain: float32 [64, 16], P('tp'), may hold values from -4 to 4
- conv_taps: float32 [3, 1024], P(None, 'tp'), may hold values from -3.5 to 3.5
- initial_state: float32 [1, 2, 64, 64], P('fs', None, 'tp'), may hold values from -6 to 6
Outputs:
- mixed: bfloat16 [1, 4096, 2048], P('fs', ('sp', 'tp'))
- final_state: float32 [1, 2, 64, 64], P('fs', None, 'tp', 'sp')
The draws below stay inside these ranges and needn't reach their ends.
All inputs are finite; a program needn't handle non-finite values.
Results may differ from the reference program's by a relative error of at most 0.018.
Values may be sent and summed in bfloat16 or wider, within the bound.
A program may use at most 64 MiB of HBM per device.

```python
import math
import jax
import jax.numpy as jnp
from jax import lax

D = 2048
GROUPS = 64
GROUP = 16
STATE = 64
CW = 1024
KW = 3
SW = 1024
SEQS = 1
LENGTH = 4096
N_TP = 2


def draw_decay_real(key, part):
    base = jax.random.fold_in(key, 7)
    key_pick, key_slow, key_fast = jax.random.split(base, 3)
    share = 0.5
    pick = jax.random.uniform(key_pick, (GROUPS, 1), jnp.float32) < share
    slow = -jnp.exp(jax.random.uniform(key_slow, (GROUPS, STATE), jnp.float32, math.log(5.0 / LENGTH), math.log(60.0 / LENGTH)))
    fast = -jnp.exp(jax.random.uniform(key_fast, (GROUPS, STATE), jnp.float32, math.log(2.0), math.log(5.0)))
    return jnp.where(pick, slow, fast)


def draw_step_rate(key, part):
    base = jax.random.fold_in(key, 13)
    key_slow, key_fine = jax.random.split(base, 2)
    blocks = LENGTH // 256
    slow = jnp.exp(jax.random.uniform(key_slow, (SEQS, blocks), jnp.float32, math.log(0.5), math.log(2.0)))
    fine = jax.random.uniform(key_fine, (SEQS, LENGTH), jnp.float32, 0.8, 1.25)
    return jnp.repeat(slow, 256, axis=1) * fine


def shard_levels(own_key, shape, cuts, smallest, top_value):
    level, own = 1.0, jax.random.fold_in(own_key, 6)
    for axis_at, parts in cuts:
        draws = jnp.exp(jax.random.uniform(jax.random.fold_in(own, axis_at), (parts,), jnp.float32, smallest / len(cuts), top_value / len(cuts)))
        level = level * jnp.repeat(draws, shape[axis_at] // parts).reshape([-1 if axis == axis_at else 1 for axis in range(len(shape))])
    return level


def noise(rng, shape, deviation, reach, pieces=(), kind=jnp.bfloat16):
    drawn = jax.random.normal(rng, shape, jnp.float32) * deviation
    if len(pieces) > 0:
        drawn = shard_levels(rng, shape, pieces, -0.22, 0.18) * drawn
    return jnp.clip(drawn, min=-reach, max=reach).astype(kind)


def setup_inputs(seed: int = 0) -> dict:
    streams_of = jax.random.split(jax.random.key(seed), 20)
    return {
        "tokens": noise(streams_of[0], (SEQS, LENGTH, D), 1.0, 6.0, ((1, 16),)),
        "norm_gain": jnp.clip(1.0 + 0.18 * jax.random.normal(streams_of[1], (D,), jnp.float32), 0.1, 1.9),
        "w_state_in": noise(streams_of[2], (D, SW), D ** -0.5, 0.125, ((0, 16), (1, 2))),
        "w_value": noise(streams_of[3], (D, CW), D ** -0.5, 0.125, ((0, 16), (1, 2))),
        "w_outer": noise(streams_of[4], (D, CW), D ** -0.5, 0.125, ((0, 16), (1, 2))),
        "w_inner": noise(streams_of[5], (D, CW), D ** -0.5, 0.125, ((0, 16), (1, 2))),
        "w_state_out": noise(streams_of[6], (D, SW), (SW + CW) ** -0.5, 0.125, ((0, 16), (1, 2))),
        "w_conv_out": noise(streams_of[7], (D, CW), (SW + CW) ** -0.5, 0.125, ((0, 16), (1, 2))),
        "log_step": jnp.clip(-4.6 + 1.3999999 * jax.random.uniform(streams_of[8], (GROUPS,), jnp.float32) ** shard_levels(streams_of[8], (GROUPS,), ((0, 2),), -0.2, 0.2), -4.6, -3.2),
        "decay_real": draw_decay_real(jax.random.fold_in(streams_of[19], 71), 0),
        "frequency": jnp.clip(1.0 + 191.0 * jax.random.uniform(streams_of[10], (GROUPS, STATE), jnp.float32) ** shard_levels(streams_of[10], (GROUPS, STATE), ((0, 2),), -0.2, 0.2), 1.0, 192.0),
        "step_rate": draw_step_rate(jax.random.fold_in(streams_of[19], 71), 0),
        "input_real": noise(streams_of[12], (GROUPS, STATE, GROUP), (2 * GROUP) ** -0.5, 1.0, ((0, 2),), jnp.float32),
        "input_imag": noise(streams_of[13], (GROUPS, STATE, GROUP), (2 * GROUP) ** -0.5, 1.0, ((0, 2),), jnp.float32),
        "read_real": noise(streams_of[14], (GROUPS, GROUP, STATE), STATE ** -0.5, 0.75, ((0, 2),), jnp.float32),
        "read_imag": noise(streams_of[15], (GROUPS, GROUP, STATE), STATE ** -0.5, 0.75, ((0, 2),), jnp.float32),
        "skip_gain": noise(streams_of[16], (GROUPS, GROUP), 1.0, 4.0, ((0, 2),), jnp.float32),
        "conv_taps": noise(streams_of[17], (KW, CW), KW ** -0.5, 3.5, ((1, 2),), jnp.float32),
        "initial_state": noise(streams_of[18], (SEQS, 2, GROUPS, STATE), 1.0, 6.0, ((2, 2),), jnp.float32),
    }


def reference(tokens, norm_gain, w_state_in, w_value, w_outer, w_inner, w_state_out, w_conv_out, log_step, decay_real, frequency, step_rate, input_real, input_imag, read_real, read_imag, skip_gain, conv_taps, initial_state):
    seqs, length, width = tokens.shape
    features = tokens.astype(jnp.float32)
    mean_square = lax.optimization_barrier(jnp.mean(features * features, axis=-1, keepdims=True))
    normed = (features * lax.rsqrt(mean_square + 1e-06) * norm_gain).astype(jnp.bfloat16).reshape(seqs * length, width)

    def project(matrix):
        return jnp.dot(normed, matrix, preferred_element_type=jnp.float32).astype(jnp.bfloat16)
    state_in = project(w_state_in)
    value = project(w_value)
    outer = project(w_outer)
    inner = project(w_inner)
    groups, states = decay_real.shape
    group = skip_gain.shape[1]
    channels = state_in.astype(jnp.float32).reshape(seqs, length, groups, group)
    step = jnp.exp(log_step)[None, None, :] * step_rate[:, :, None]
    modulus = decay_real * decay_real + frequency * frequency

    def advance(carry, inputs):
        hidden_real, hidden_imag = carry
        chan_now, step_now = inputs
        scaled = step_now[..., None]
        grow = jnp.exp(scaled * decay_real)
        angle = scaled * frequency
        bar_real = grow * jnp.cos(angle)
        bar_imag = grow * jnp.sin(angle)
        less_real = bar_real - 1.0
        hold_real = (less_real * decay_real + bar_imag * frequency) / modulus
        hold_imag = (bar_imag * decay_real - less_real * frequency) / modulus
        drive_real = jnp.einsum('sgh,gph->sgp', chan_now, input_real, precision=lax.Precision.HIGHEST)
        drive_imag = jnp.einsum('sgh,gph->sgp', chan_now, input_imag, precision=lax.Precision.HIGHEST)
        push_real = hold_real * drive_real - hold_imag * drive_imag
        push_imag = hold_real * drive_imag + hold_imag * drive_real
        next_real = bar_real * hidden_real - bar_imag * hidden_imag + push_real
        next_imag = bar_real * hidden_imag + bar_imag * hidden_real + push_imag
        response = jnp.einsum('sgp,ghp->sgh', next_real, read_real, precision=lax.Precision.HIGHEST) - jnp.einsum('sgp,ghp->sgh', next_imag, read_imag, precision=lax.Precision.HIGHEST) + skip_gain * chan_now
        return ((next_real, next_imag), response)
    (last_real, last_imag), responses = lax.scan(advance, (initial_state[:, 0], initial_state[:, 1]), (channels.transpose(1, 0, 2, 3), step.transpose(1, 0, 2)))
    state_mix = jax.nn.gelu(responses.transpose(1, 0, 2, 3)).reshape(seqs * length, groups * group).astype(jnp.bfloat16)
    final_state = jnp.stack([last_real, last_imag], axis=1)
    gated = (inner.astype(jnp.float32) * value.astype(jnp.float32)).astype(jnp.bfloat16).reshape(seqs, length, -1)
    taps = conv_taps.shape[0]
    padded = jnp.pad(gated, ((0, 0), (taps - 1, 0), (0, 0))).astype(jnp.float32)
    filtered = jnp.zeros((seqs, length, gated.shape[2]), jnp.float32)
    for tap in range(taps):
        filtered = filtered + conv_taps[tap] * padded[:, tap:tap + length]
    conv_mix = (outer.astype(jnp.float32).reshape(seqs, length, -1) * filtered).astype(jnp.bfloat16).reshape(seqs * length, -1)
    state_block = state_mix.shape[1] // N_TP
    conv_block = conv_mix.shape[1] // N_TP
    total = jnp.zeros((seqs * length, width), jnp.float32)
    for block in range(N_TP):
        part = jnp.dot(state_mix[:, block * state_block:(block + 1) * state_block], w_state_out[:, block * state_block:(block + 1) * state_block].T, preferred_element_type=jnp.float32) + jnp.dot(conv_mix[:, block * conv_block:(block + 1) * conv_block], w_conv_out[:, block * conv_block:(block + 1) * conv_block].T, preferred_element_type=jnp.float32)
        total = total + lax.optimization_barrier(part.astype(jnp.bfloat16)).astype(jnp.float32)
    mixed = total.astype(jnp.bfloat16).reshape(seqs, length, width)
    return (mixed, final_state)
```

```python
import jax
import jax.numpy as jnp
from jax import lax
from jax.experimental import pallas as pl
from jax.experimental.pallas import tpu as pltpu
from jax.sharding import PartitionSpec as P

F32 = jnp.float32
BF16 = jnp.bfloat16
SUB = 8
SIN = (3.1415925798055846, -5.16770686616794, 2.5500311935192803, -0.5980441939118888, 0.07721838615680923)
COS = (0.9999999997799038, -4.93480213707883, 4.058709159556464, -1.335212003052184, 0.2349373138245546, -0.024396324364378108)


def poly(coeffs, z):
    total = coeffs[-1]
    for c in coeffs[-2::-1]:
        total = total * z + c
    return total


def dot(a, b, dims=((1,), (0,))):
    return lax.dot_general(a, b, (dims, ((), ())), preferred_element_type=F32)


def iota(shape, dim):
    return lax.broadcasted_iota(jnp.int32, shape, dim)


def cmul(ar, ai, br, bi):
    return ar * br - ai * bi, ar * bi + ai * br


def permutation(rows):
    run = rows // SUB
    r, t = iota((rows, rows), 0), iota((rows, rows), 1)
    return jnp.where((r % SUB) * run + r // SUB == t, 1.0, 0.0).astype(BF16)


def couple(block, state_p, in_r, in_i, dr_ref, di_ref, group, states):
    width = state_p.shape[1]
    span = width // group * states
    rows = slice(block * span, (block + 1) * span)
    tile = jnp.where(iota((group, width), 0) == iota((group, width), 1) % group, 1.0, 0.0).astype(BF16)
    keep = iota((span, width), 0) // states == iota((span, width), 1) // group
    for src, dst in ((in_r, dr_ref), (in_i, di_ref)):
        full = jnp.where(keep, dot(src[rows, :], tile), 0.0).astype(BF16)
        dst[:, rows] = dot(state_p, full, ((1,), (1,)))


def scan_block(lo, span, rate, coef, hr, hi, ar, ai):
    cols = pl.ds(lo, span)
    run = rate.shape[0] // SUB
    reps = span // 128
    decay = jnp.broadcast_to(coef[0:1, cols], (SUB, span))
    turn = jnp.broadcast_to(coef[1:2, cols], (SUB, span))

    def one(j, carry):
        h_r, h_i, a_r, a_i = carry
        at = pl.ds(pl.multiple_of(j * SUB, SUB), SUB)
        r = jnp.concatenate([rate[at, :]] * reps, axis=1)
        u = r * turn
        f = u - jnp.floor(u + 0.5)
        z = f * f
        s = f * poly(SIN, z)
        c = poly(COS, z)
        grow = jnp.exp(r * decay)
        gs = 2.0 * grow * s
        b_r = grow - gs * s
        b_i = gs * c
        p_r, p_i = cmul(b_r - 1.0, b_i, hr[at, cols], hi[at, cols])
        m_r, m_i = cmul(b_r, b_i, h_r, h_i)
        h_r, h_i = m_r + p_r, m_i + p_i
        a_r, a_i = cmul(b_r, b_i, a_r, a_i)
        hr[at, cols] = h_r
        hi[at, cols] = h_i
        ar[at, cols] = a_r
        ai[at, cols] = a_i
        return h_r, h_i, a_r, a_i

    zero = jnp.zeros((SUB, span), F32)
    lax.fori_loop(0, run, one, (zero, zero, zero + 1.0, zero), unroll=2)


def chain_subs(hr, hi, ar, ai, pre, summ):
    rows, flat = hr.shape
    last = rows - SUB
    m_r, m_i = jnp.ones((1, flat), F32), jnp.zeros((1, flat), F32)
    v_r, v_i = jnp.zeros((1, flat), F32), jnp.zeros((1, flat), F32)
    for s in range(SUB):
        row = slice(s, s + 1)
        pre[0, row, :], pre[1, row, :], pre[2, row, :], pre[3, row, :] = m_r, m_i, v_r, v_i
        at = slice(last + s, last + s + 1)
        e_r, e_i = ar[at, :], ai[at, :]
        m_r, m_i = cmul(e_r, e_i, m_r, m_i)
        w_r, w_i = cmul(e_r, e_i, v_r, v_i)
        v_r, v_i = w_r + hr[at, :], w_i + hi[at, :]
    summ[0:1, :], summ[1:2, :], summ[2:3, :], summ[3:4, :] = m_r, m_i, v_r, v_i


def enter_states(place, count, get, opening):
    s_r, s_i = opening[0:1, :], opening[1:2, :]
    e_r, e_i = s_r, s_i
    for j in range(count):
        g = get(j)
        here = place == j
        e_r, e_i = jnp.where(here, s_r, e_r), jnp.where(here, s_i, e_i)
        t_r, t_i = cmul(g[0:1, :], g[1:2, :], s_r, s_i)
        s_r, s_i = t_r + g[2:3, :], t_i + g[3:4, :]
    return e_r, e_i, s_r, s_i


def readout(block, width, state_p, enter, hr, hi, ar, ai, pre, rd_r, rd_i, skip, perm, out, group, states):
    span = width // group * states
    cols = slice(block * span, (block + 1) * span)
    chans = slice(block * width, (block + 1) * width)
    rows = hr.shape[0]
    run = rows // SUB
    e_r, e_i = cmul(pre[0, :, cols], pre[1, :, cols], enter[0][:, cols], enter[1][:, cols])
    e_r, e_i = e_r + pre[2, :, cols], e_i + pre[3, :, cols]
    tile = jnp.where(iota((states, span), 0) == iota((states, span), 1) % states, 1.0, 0.0).astype(BF16)
    keep = iota((width, span), 0) // group == iota((width, span), 1) // states
    g_r = jnp.where(keep, dot(rd_r[chans, :], tile), 0.0).astype(BF16)
    g_i = jnp.where(keep, dot(rd_i[chans, :], tile), 0.0).astype(BF16)

    def fixed(local, a, b, sign):
        a3, b3 = a[:, cols].reshape(run, SUB, span), b[:, cols].reshape(run, SUB, span)
        x, y = (e_r, e_i) if sign < 0 else (e_i, e_r)
        shift = a3 * x[None] + (b3 * y[None] if sign > 0 else -b3 * y[None])
        return (local[:, cols].reshape(run, SUB, span) + shift).reshape(rows, span).astype(BF16)

    total = dot(fixed(hr, ar, ai, -1), g_r, ((1,), (1,))) - dot(fixed(hi, ar, ai, 1), g_i, ((1,), (1,)))
    v = total + skip[:, chans] * state_p[:, chans].astype(F32)
    mix = 0.5 * v * (1.0 + jnp.tanh(0.7978845608 * (v + 0.044715 * (v * v * v))))
    out[:, chans] = dot(perm, mix.astype(BF16), ((0,), (0,))).astype(BF16)


def ssm_prepare(log_step, decay_real, frequency, step_rate, input_real, input_imag, read_real, read_imag, skip_gain, initial_state, rows):
    groups, states = decay_real.shape
    group = skip_gain.shape[1]
    flat = groups * states
    base = jnp.exp(log_step)[:, None]
    coef = jnp.stack([base * decay_real, base * frequency * 0.15915494309189535]).reshape(2, flat)
    modulus = decay_real * decay_real + frequency * frequency
    inv_r, inv_i = (decay_real / modulus)[..., None], (-frequency / modulus)[..., None]
    in_r = (input_real * inv_r - input_imag * inv_i).astype(BF16).reshape(flat, group)
    in_i = (input_real * inv_i + input_imag * inv_r).astype(BF16).reshape(flat, group)
    rd_r = read_real.astype(BF16).reshape(groups * group, states)
    rd_i = read_imag.astype(BF16).reshape(groups * group, states)
    rate = jnp.broadcast_to(step_rate[0].reshape(SUB, rows // SUB).T.reshape(rows, 1), (rows, 128))
    return coef, rate, in_r, in_i, rd_r, rd_i, skip_gain.reshape(1, groups * group), initial_state[0].reshape(2, flat)


def local_kernel(group, states, state_in, rate, coef, in_r, in_i, hr, hi, ar, ai, pre, summ, state_p):
    perm = permutation(state_in.shape[0])
    state_p[...] = dot(perm, state_in[...]).astype(BF16)
    channels = state_in.shape[1]
    width = min(128, channels)
    span = width // group * states
    for block in range(channels // width):
        couple(block, state_p[:, block * width : (block + 1) * width], in_r, in_i, hr, hi, group, states)
        scan_block(block * span, span, rate, coef, hr, hi, ar, ai)
    chain_subs(hr, hi, ar, ai, pre, summ)


def read_kernel(group, states, gathered, opening, hr, hi, ar, ai, pre, state_p, rd_r, rd_i, skip, out, final):
    place = lax.axis_index("sp")
    e_r, e_i, s_r, s_i = enter_states(place, gathered.shape[0], lambda j: gathered[j], opening)
    final[0:1, :] = s_r
    final[1:2, :] = s_i
    perm = permutation(hr.shape[0])
    channels = out.shape[1]
    width = min(128, channels)
    for block in range(channels // width):
        readout(block, width, state_p, (e_r, e_i), hr, hi, ar, ai, pre, rd_r, rd_i, skip, perm, out, group, states)


def body(tokens, norm_gain, w_state_in, w_value, w_outer, w_inner, w_state_out, w_conv_out, log_step, decay_real, frequency, step_rate, input_real, input_imag, read_real, read_imag, skip_gain, conv_taps, initial_state):
    rows = tokens.shape[1]
    groups, states = decay_real.shape
    group = skip_gain.shape[1]
    flat = groups * states
    channels = groups * group
    features = tokens[0].astype(F32)
    mean_square = jnp.mean(features * features, axis=-1, keepdims=True)
    normed = (features * lax.rsqrt(mean_square + 1e-06) * norm_gain).astype(BF16)
    conv = conv_taps.shape[1]
    first = lax.all_gather(w_state_in, ("sp", "fs"), axis=0, tiled=True)
    rest = lax.all_gather(
        jnp.concatenate([w_value, w_inner, w_outer, w_state_out, w_conv_out], axis=1), ("sp", "fs"), axis=0, tiled=True
    )
    coef, rate, in_r, in_i, rd_r, rd_i, skip, opening = ssm_prepare(
        log_step, decay_real, frequency, step_rate, input_real, input_imag, read_real, read_imag, skip_gain, initial_state, rows
    )
    state_in = jnp.dot(normed, first, preferred_element_type=F32).astype(BF16)
    big = jax.ShapeDtypeStruct((rows, flat), F32)
    vmem = pl.BlockSpec(memory_space=pltpu.VMEM)
    cost = pl.CostEstimate(flops=20_000_000_0, bytes_accessed=1 << 23, transcendentals=0)
    hr, hi, ar, ai, pre, summ, state_p = pl.pallas_call(
        lambda *refs: local_kernel(group, states, *refs),
        out_shape=(big, big, big, big, jax.ShapeDtypeStruct((4, SUB, flat), F32), jax.ShapeDtypeStruct((4, flat), F32), jax.ShapeDtypeStruct((rows, channels), BF16)),
        in_specs=[vmem] * 5,
        out_specs=[vmem] * 7,
        cost_estimate=cost,
        name="local_scan",
    )(state_in, rate, coef, in_r, in_i)
    gathered = lax.all_gather(summ, "sp")
    state_mix, final = pl.pallas_call(
        lambda *refs: read_kernel(group, states, *refs),
        out_shape=(jax.ShapeDtypeStruct((rows, channels), BF16), jax.ShapeDtypeStruct((2, flat), F32)),
        in_specs=[vmem] * 11,
        out_specs=[vmem] * 2,
        cost_estimate=cost,
        name="read_out",
    )(gathered, opening, hr, hi, ar, ai, pre, state_p, rd_r, rd_i, skip)

    def project(k):
        return jnp.dot(normed, rest[:, k * conv : (k + 1) * conv], preferred_element_type=F32).astype(BF16)

    value, inner, outer = project(0), project(1), project(2)
    gated = (inner.astype(F32) * value.astype(F32)).astype(BF16)
    reach = conv_taps.shape[0] - 1
    count = lax.axis_size("sp")
    earlier = lax.ppermute(gated[rows - reach :], "sp", [(k, k + 1) for k in range(count - 1)])
    extended = jnp.concatenate([earlier, gated], axis=0).astype(F32)
    filtered = conv_taps[0] * extended[0:rows]
    for tap in range(1, reach + 1):
        filtered = filtered + conv_taps[tap] * extended[tap : tap + rows]
    conv_mix = (outer.astype(F32) * filtered).astype(BF16)
    w_so = rest[:, 3 * conv : 3 * conv + channels]
    w_co = rest[:, 3 * conv + channels :]
    partial = jnp.einsum("rc,dc->rd", state_mix, w_so, preferred_element_type=F32) + jnp.einsum(
        "rc,dc->rd", conv_mix, w_co, preferred_element_type=F32
    )
    mixed = lax.psum_scatter(partial.astype(BF16), "tp", scatter_dimension=0, tiled=True)
    share = states // count
    own = lax.dynamic_slice_in_dim(final.reshape(2, groups, states), lax.axis_index("sp") * share, share, 2)
    return mixed[None], own[None]


def solution(mesh):
    return jax.shard_map(
        body,
        mesh=mesh,
        in_specs=(
            P("fs", "sp", None),
            P(),
            P(("sp", "fs"), "tp"),
            P(("sp", "fs"), "tp"),
            P(("sp", "fs"), "tp"),
            P(("sp", "fs"), "tp"),
            P(("sp", "fs"), "tp"),
            P(("sp", "fs"), "tp"),
            P("tp"),
            P("tp", None),
            P("tp", None),
            P("fs", "sp"),
            P("tp", None, None),
            P("tp", None, None),
            P("tp", None, None),
            P("tp", None, None),
            P("tp", None),
            P(None, "tp"),
            P("fs", None, "tp", None),
        ),
        out_specs=(P("fs", ("sp", "tp"), None), P("fs", None, "tp", "sp")),
        check_vma=False,
    )
```

```python
import jax
import jax.numpy as jnp
from jax import lax
from jax.experimental import pallas as pl
from jax.experimental.pallas import tpu as pltpu
from jax.sharding import PartitionSpec as P

F32 = jnp.float32
BF16 = jnp.bfloat16
SUB = 8
SIN = (3.1415925798055846, -5.16770686616794, 2.5500311935192803, -0.5980441939118888, 0.07721838615680923)
COS = (0.9999999997799038, -4.93480213707883, 4.058709159556464, -1.335212003052184, 0.2349373138245546, -0.024396324364378108)


def poly(coeffs, z):
    total = coeffs[-1]
    for c in coeffs[-2::-1]:
        total = total * z + c
    return total


def dot(a, b, dims=((1,), (0,))):
    return lax.dot_general(a, b, (dims, ((), ())), preferred_element_type=F32)


def iota(shape, dim):
    return lax.broadcasted_iota(jnp.int32, shape, dim)


def cmul(ar, ai, br, bi):
    return ar * br - ai * bi, ar * bi + ai * br


def permutation(rows):
    run = rows // SUB
    r, t = iota((rows, rows), 0), iota((rows, rows), 1)
    return jnp.where((r % SUB) * run + r // SUB == t, 1.0, 0.0).astype(BF16)


def couple(block, state_p, in_r, in_i, dr_ref, di_ref, group, states):
    width = state_p.shape[1]
    span = width // group * states
    rows = slice(block * span, (block + 1) * span)
    tile = jnp.where(iota((group, width), 0) == iota((group, width), 1) % group, 1.0, 0.0).astype(BF16)
    keep = iota((span, width), 0) // states == iota((span, width), 1) // group
    for src, dst in ((in_r, dr_ref), (in_i, di_ref)):
        full = jnp.where(keep, dot(src[rows, :], tile), 0.0).astype(BF16)
        dst[:, rows] = dot(state_p, full, ((1,), (1,)))


def scan_block(lo, span, rate, coef, hr, hi, ar, ai):
    cols = pl.ds(lo, span)
    run = rate.shape[0] // SUB
    reps = span // 128
    decay = jnp.broadcast_to(coef[0:1, cols], (SUB, span))
    turn = jnp.broadcast_to(coef[1:2, cols], (SUB, span))

    def one(j, carry):
        h_r, h_i, a_r, a_i = carry
        at = pl.ds(pl.multiple_of(j * SUB, SUB), SUB)
        r = jnp.concatenate([rate[at, :]] * reps, axis=1)
        u = r * turn
        f = u - jnp.floor(u + 0.5)
        z = f * f
        s = f * poly(SIN, z)
        c = poly(COS, z)
        grow = jnp.exp(r * decay)
        gs = 2.0 * grow * s
        b_r = grow - gs * s
        b_i = gs * c
        p_r, p_i = cmul(b_r - 1.0, b_i, hr[at, cols], hi[at, cols])
        m_r, m_i = cmul(b_r, b_i, h_r, h_i)
        h_r, h_i = m_r + p_r, m_i + p_i
        a_r, a_i = cmul(b_r, b_i, a_r, a_i)
        hr[at, cols] = h_r
        hi[at, cols] = h_i
        ar[at, cols] = a_r
        ai[at, cols] = a_i
        return h_r, h_i, a_r, a_i

    zero = jnp.zeros((SUB, span), F32)
    lax.fori_loop(0, run, one, (zero, zero, zero + 1.0, zero), unroll=2)


def chain_subs(hr, hi, ar, ai, pre, summ):
    rows, flat = hr.shape
    last = rows - SUB
    m_r, m_i = jnp.ones((1, flat), F32), jnp.zeros((1, flat), F32)
    v_r, v_i = jnp.zeros((1, flat), F32), jnp.zeros((1, flat), F32)
    for s in range(SUB):
        row = slice(s, s + 1)
        pre[0, row, :], pre[1, row, :], pre[2, row, :], pre[3, row, :] = m_r, m_i, v_r, v_i
        at = slice(last + s, last + s + 1)
        e_r, e_i = ar[at, :], ai[at, :]
        m_r, m_i = cmul(e_r, e_i, m_r, m_i)
        w_r, w_i = cmul(e_r, e_i, v_r, v_i)
        v_r, v_i = w_r + hr[at, :], w_i + hi[at, :]
    summ[0:1, :], summ[1:2, :], summ[2:3, :], summ[3:4, :] = m_r, m_i, v_r, v_i


def enter_states(place, count, get, opening):
    s_r, s_i = opening[0:1, :], opening[1:2, :]
    e_r, e_i = s_r, s_i
    for j in range(count):
        g = get(j)
        here = place == j
        e_r, e_i = jnp.where(here, s_r, e_r), jnp.where(here, s_i, e_i)
        t_r, t_i = cmul(g[0:1, :], g[1:2, :], s_r, s_i)
        s_r, s_i = t_r + g[2:3, :], t_i + g[3:4, :]
    return e_r, e_i, s_r, s_i


def readout(block, width, state_p, enter, hr, hi, ar, ai, pre, rd_r, rd_i, skip, perm, out, group, states):
    span = width // group * states
    cols = slice(block * span, (block + 1) * span)
    chans = slice(block * width, (block + 1) * width)
    rows = hr.shape[0]
    run = rows // SUB
    e_r, e_i = cmul(pre[0, :, cols], pre[1, :, cols], enter[0][:, cols], enter[1][:, cols])
    e_r, e_i = e_r + pre[2, :, cols], e_i + pre[3, :, cols]
    tile = jnp.where(iota((states, span), 0) == iota((states, span), 1) % states, 1.0, 0.0).astype(BF16)
    keep = iota((width, span), 0) // group == iota((width, span), 1) // states
    g_r = jnp.where(keep, dot(rd_r[chans, :], tile), 0.0).astype(BF16)
    g_i = jnp.where(keep, dot(rd_i[chans, :], tile), 0.0).astype(BF16)

    def fixed(local, a, b, sign):
        a3, b3 = a[:, cols].reshape(run, SUB, span), b[:, cols].reshape(run, SUB, span)
        x, y = (e_r, e_i) if sign < 0 else (e_i, e_r)
        shift = a3 * x[None] + (b3 * y[None] if sign > 0 else -b3 * y[None])
        return (local[:, cols].reshape(run, SUB, span) + shift).reshape(rows, span).astype(BF16)

    total = dot(fixed(hr, ar, ai, -1), g_r, ((1,), (1,))) - dot(fixed(hi, ar, ai, 1), g_i, ((1,), (1,)))
    v = total + skip[:, chans] * state_p[:, chans].astype(F32)
    mix = 0.5 * v * (1.0 + jnp.tanh(0.7978845608 * (v + 0.044715 * (v * v * v))))
    out[:, chans] = dot(perm, mix.astype(BF16), ((0,), (0,))).astype(BF16)


def ssm_prepare(log_step, decay_real, frequency, step_rate, input_real, input_imag, read_real, read_imag, skip_gain, initial_state, rows):
    groups, states = decay_real.shape
    group = skip_gain.shape[1]
    flat = groups * states
    base = jnp.exp(log_step)[:, None]
    coef = jnp.stack([base * decay_real, base * frequency * 0.15915494309189535]).reshape(2, flat)
    modulus = decay_real * decay_real + frequency * frequency
    inv_r, inv_i = (decay_real / modulus)[..., None], (-frequency / modulus)[..., None]
    in_r = (input_real * inv_r - input_imag * inv_i).astype(BF16).reshape(flat, group)
    in_i = (input_real * inv_i + input_imag * inv_r).astype(BF16).reshape(flat, group)
    rd_r = read_real.astype(BF16).reshape(groups * group, states)
    rd_i = read_imag.astype(BF16).reshape(groups * group, states)
    rate = jnp.broadcast_to(step_rate[0].reshape(SUB, rows // SUB).T.reshape(rows, 1), (rows, 128))
    return coef, rate, in_r, in_i, rd_r, rd_i, skip_gain.reshape(1, groups * group), initial_state[0].reshape(2, flat)


MESH = pl.DeviceIdType.MESH
HALO = 16
S, V, I, O, SO, CO = range(6)


def layer_kernel(
    sizes, tokens, gain, w_0, w_1, w_2, w_3, w_4, w_5, rate, coef, in_r, in_i, rd_r, rd_i, skip, taps, opening,
    out, final,
    full, normed, state_p, hr, hi, ar, ai, pre, summ, sums, ext, halo_src, halo_dst, conv_mix, state_mix, partial, got,
    ring_send, ring_recv, sib_send, sib_recv, sum_send, sum_recv, x_send, x_recv, halo_send, halo_recv,
):
    n_sp, n_fs, n_tp, group, states = sizes
    weights = (w_0, w_1, w_2, w_3, w_4, w_5)
    shard = w_0.shape[0]
    rows = tokens.shape[0]
    channels = w_0.shape[1]
    sp, fs, tp = lax.axis_index("sp"), lax.axis_index("fs"), lax.axis_index("tp")
    pairs = n_sp * n_fs // 2
    half = pairs // 2
    mine = sp * n_fs + fs
    parity, chip = mine % 2, mine // 2
    place = jnp.where(chip % 2 == 0, chip // 2, pairs - 1 - chip // 2)

    def pair_at(offset):
        q = (place + offset + pairs) % pairs
        return jnp.where(q < half, q * 2, (pairs - 1 - q) * 2 + 1)

    def device(linear):
        return (linear // n_fs, linear % n_fs, tp)

    neighbours = (device(pair_at(1) * 2 + parity), device(pair_at(-1) * 2 + parity))
    sibling = device(chip * 2 + 1 - parity)
    sp_peers = [((sp + s) % n_sp, fs, tp) for s in range(1, n_sp)]
    tp_peers = [(sp, fs, (tp + s) % n_tp) for s in range(1, n_tp)]

    barrier = pltpu.get_barrier_semaphore()
    greet = list(neighbours) + [sibling] + sp_peers + tp_peers
    for other in greet:
        pl.semaphore_signal(barrier, inc=1, device_id=other, device_id_type=MESH)
    pl.semaphore_wait(barrier, len(greet))

    sent = []

    def send(src, dst, s_sem, r_sem, to):
        copy = pltpu.make_async_remote_copy(src_ref=src, dst_ref=dst, send_sem=s_sem, recv_sem=r_sem, device_id=to, device_id_type=MESH)
        copy.start()
        sent.append(copy)

    def landed(ref, s_sem, r_sem):
        pltpu.make_async_remote_copy(
            src_ref=ref, dst_ref=ref, send_sem=s_sem, recv_sem=r_sem, device_id=sibling, device_id_type=MESH
        ).wait_recv()

    def slot(w, pair, par):
        return full.at[w, pl.ds(pl.multiple_of((pair * 2 + par) * shard, shard), shard), :]

    def rounds(w, way):
        return half if way == w % 2 else pairs - 1 - half

    def source(way, r):
        return pair_at(-1 - r if way == 0 else 1 + r)

    arrived = set()
    shared = set()

    def arrive(w, way, r):
        if (w, way, r) in arrived:
            return
        arrived.add((w, way, r))
        ref = slot(w, source(way, r), parity)
        landed(ref, ring_send.at[w, way, r], ring_recv.at[w, way, r])
        d = 1 + way * half + r
        send(ref, ref, sib_send.at[w, d], sib_recv.at[w, d], sibling)

    def share(w, d, pair):
        if (w, d) not in shared:
            shared.add((w, d))
            landed(slot(w, pair, 1 - parity), sib_send.at[w, d], sib_recv.at[w, d])

    def issue(w, r):
        for way in range(2):
            if r >= rounds(w, way):
                continue
            if r == 0:
                src, at = weights[w], chip
            else:
                arrive(w, way, r - 1)
                at = source(way, r - 1)
                src = slot(w, at, parity)
            send(src, slot(w, at, parity), ring_send.at[w, way, r], ring_recv.at[w, way, r], neighbours[way])
        if r == 0:
            send(weights[w], slot(w, chip, parity), sib_send.at[w, 0], sib_recv.at[w, 0], sibling)
            full[w, pl.ds(pl.multiple_of(mine * shard, shard), shard), :] = weights[w][...]

    def finish(w):
        for r in range(half):
            for way in range(2):
                if r < rounds(w, way):
                    arrive(w, way, r)
        share(w, 0, chip)
        for r in range(half):
            for way in range(2):
                if r < rounds(w, way):
                    share(w, 1 + way * half + r, source(way, r))

    queue = [(S, 0), (V, 0), (S, 1), (I, 0), (S, 2), (O, 0)]
    for r in range(3, half):
        queue += [(S, r), (V, r - 2), (I, r - 2)]
    todo = [(w, r) for r in range(half) for w in (V, I, O) if (w, r) not in queue]
    todo_out = [(w, r) for r in range(half) for w in (SO, CO)]
    at_once = todo[:-2] + todo_out[:1] + todo[-2:-1] + todo_out[1:2] + todo[-1:] + todo_out[2:]
    queue += at_once
    done = [0]

    def advance(count):
        count = max(0, min(count, len(queue) - done[0]))
        for w, r in queue[done[0] : done[0] + count]:
            issue(w, r)
        done[0] += count

    def until(w, r):
        advance(queue.index((w, r)) + 1 - done[0])

    advance(2)

    def norm(j, carry):
        at = pl.ds(pl.multiple_of(j * 32, 32), 32)
        x = tokens[at, :].astype(F32)
        scale = lax.rsqrt(jnp.mean(x * x, axis=-1, keepdims=True) + 1e-06)
        normed[at, :] = (x * scale * gain[...]).astype(BF16)
        return carry

    lax.fori_loop(0, rows // 32, norm, 0)
    perm = permutation(rows)
    until(S, half - 1)
    advance(2)
    finish(S)

    def project(w):
        return dot(normed[...], full[w]).astype(BF16)

    state_p[...] = dot(perm, project(S)).astype(BF16)
    width = min(128, channels)
    span = width // group * states
    blocks = channels // width
    for block in range(blocks):
        couple(block, state_p[:, block * width : (block + 1) * width], in_r, in_i, hr, hi, group, states)
        scan_block(block * span, span, rate, coef, hr, hi, ar, ai)
        advance(1)
    chain_subs(hr, hi, ar, ai, pre, summ)
    until(V, half - 1)
    finish(V)
    value = project(V)
    for s, other in enumerate(sp_peers):
        send(summ, sums.at[sp], sum_send.at[s], sum_recv.at[s], other)
    sums[pl.ds(sp, 1)] = summ[...][None]
    until(I, half - 1)
    finish(I)
    product = (project(I).astype(F32) * value.astype(F32)).astype(BF16)
    halo_src[...] = product[rows - HALO :, :]
    ext[HALO:, :] = product.astype(F32)
    until(O, half - 1)
    finish(O)
    outer = project(O)
    send(halo_src, halo_dst, halo_send, halo_recv, ((sp + 1) % n_sp, fs, tp))
    advance(1)
    landed(halo_dst, halo_send, halo_recv)
    ext[:HALO, :] = jnp.where(sp == 0, 0.0, halo_dst[...].astype(F32))
    reach = taps.shape[0] - 1
    filtered = taps[0:1, :] * ext[HALO - reach : HALO - reach + rows, :]
    for tap in range(1, reach + 1):
        at = HALO - reach + tap
        filtered = filtered + taps[tap : tap + 1, :] * ext[at : at + rows, :]
    conv_mix[...] = (outer.astype(F32) * filtered).astype(BF16)
    advance(1)
    for s in range(1, n_sp):
        landed(sums.at[(sp + n_sp - s) % n_sp], sum_send.at[s - 1], sum_recv.at[s - 1])
    e_r, e_i, s_r, s_i = enter_states(sp, n_sp, lambda j: sums[j], opening)
    final[0:1, :] = s_r
    final[1:2, :] = s_i
    for block in range(blocks):
        readout(block, width, state_p, (e_r, e_i), hr, hi, ar, ai, pre, rd_r, rd_i, skip, perm, state_mix, group, states)
        advance(1)
    own_rows = rows // n_tp
    chunks = []

    def compute(pair):
        c = len(chunks)
        at = pl.ds(pl.multiple_of(pair * 2 * shard, 2 * shard), 2 * shard)
        partial[pl.ds(pair, 1)] = (
            dot(state_mix[...], full[SO, at, :], ((1,), (1,))) + dot(conv_mix[...], full[CO, at, :], ((1,), (1,)))
        ).astype(BF16)[None]
        chunks.append(pair)
        if c > 0:
            exchange(c - 1)

    def exchange(c):
        pair = chunks[c]
        for s, other in enumerate(tp_peers):
            theirs = pl.ds(pl.multiple_of(other[2] * own_rows, own_rows), own_rows)
            send(partial.at[pair, theirs, :], got.at[pair, s], x_send.at[c, s], x_recv.at[c, s], other)

    share(SO, 0, chip)
    share(CO, 0, chip)
    compute(chip)
    for r in range(half - 1):
        for w in (SO, CO):
            until(w, r + 1)
        for way in range(2):
            for w in (SO, CO):
                arrive(w, way, r)
            for w in (SO, CO):
                share(w, 1 + way * half + r, source(way, r))
            compute(source(way, r))
    for w in (SO, CO):
        arrive(w, w % 2, half - 1)
    for w in (SO, CO):
        share(w, 1 + (w % 2) * half + half - 1, source(w % 2, half - 1))
    compute(source(0, half - 1))
    exchange(len(chunks) - 1)
    kept = pl.ds(pl.multiple_of(tp * own_rows, own_rows), own_rows)
    for c, pair in enumerate(chunks):
        for s in range(n_tp - 1):
            landed(got.at[pair, s], x_send.at[c, s], x_recv.at[c, s])
    for k in range(pairs):
        total = partial[k, kept, :].astype(F32)
        for s in range(n_tp - 1):
            total = total + got[k, s].astype(F32)
        out[:, k * 2 * shard : (k + 1) * 2 * shard] = total.astype(BF16)
    for copy in sent:
        copy.wait_send()


def body(tokens, norm_gain, w_state_in, w_value, w_outer, w_inner, w_state_out, w_conv_out, log_step, decay_real, frequency, step_rate, input_real, input_imag, read_real, read_imag, skip_gain, conv_taps, initial_state):
    rows, features = tokens.shape[1:]
    groups, states = decay_real.shape
    group = skip_gain.shape[1]
    flat = groups * states
    channels = groups * group
    conv = conv_taps.shape[1]
    n_sp, n_fs, n_tp = (lax.axis_size(a) for a in ("sp", "fs", "tp"))
    shard = w_state_in.shape[0]
    pairs = n_sp * n_fs // 2
    half = pairs // 2
    coef, rate, in_r, in_i, rd_r, rd_i, skip, opening = ssm_prepare(
        log_step, decay_real, frequency, step_rate, input_real, input_imag, read_real, read_imag, skip_gain, initial_state, rows
    )
    vmem = pl.BlockSpec(memory_space=pltpu.VMEM)
    dma = pltpu.SemaphoreType.DMA
    out, final = pl.pallas_call(
        lambda *refs: layer_kernel((n_sp, n_fs, n_tp, group, states), *refs),
        out_shape=(jax.ShapeDtypeStruct((rows // n_tp, features), BF16), jax.ShapeDtypeStruct((2, flat), F32)),
        in_specs=[vmem] * 17,
        out_specs=[vmem] * 2,
        scratch_shapes=[
            pltpu.VMEM((6, n_sp * n_fs * shard, channels), BF16),
            pltpu.VMEM((rows, features), BF16),
            pltpu.VMEM((rows, channels), BF16),
            *[pltpu.VMEM((rows, flat), F32)] * 4,
            pltpu.VMEM((4, SUB, flat), F32),
            pltpu.VMEM((4, flat), F32),
            pltpu.VMEM((n_sp, 4, flat), F32),
            pltpu.VMEM((rows + HALO, conv), F32),
            pltpu.VMEM((HALO, conv), BF16),
            pltpu.VMEM((HALO, conv), BF16),
            pltpu.VMEM((rows, conv), BF16),
            pltpu.VMEM((rows, channels), BF16),
            pltpu.VMEM((pairs, rows, 2 * shard), BF16),
            pltpu.VMEM((pairs, n_tp - 1, rows // n_tp, 2 * shard), BF16),
            dma((6, 2, half)),
            dma((6, 2, half)),
            dma((6, 1 + 2 * half)),
            dma((6, 1 + 2 * half)),
            dma((n_sp - 1,)),
            dma((n_sp - 1,)),
            dma((pairs, n_tp - 1)),
            dma((pairs, n_tp - 1)),
            dma,
            dma,
        ],
        compiler_params=pltpu.CompilerParams(collective_id=0, has_side_effects=True, vmem_limit_bytes=60000 * 1024),
        name="layer",
    )(
        tokens[0], norm_gain[None], w_state_in, w_value, w_inner, w_outer, w_state_out, w_conv_out,
        rate, coef, in_r, in_i, rd_r, rd_i, skip, conv_taps, opening,
    )
    share = states // n_sp
    own = lax.dynamic_slice_in_dim(final.reshape(2, groups, states), lax.axis_index("sp") * share, share, 2)
    return out[None], own[None]


def solution(mesh):
    return jax.shard_map(
        body,
        mesh=mesh,
        in_specs=(
            P("fs", "sp", None),
            P(),
            P(("sp", "fs"), "tp"),
            P(("sp", "fs"), "tp"),
            P(("sp", "fs"), "tp"),
            P(("sp", "fs"), "tp"),
            P(("sp", "fs"), "tp"),
            P(("sp", "fs"), "tp"),
            P("tp"),
            P("tp", None),
            P("tp", None),
            P("fs", "sp"),
            P("tp", None, None),
            P("tp", None, None),
            P("tp", None, None),
            P("tp", None, None),
            P("tp", None),
            P(None, "tp"),
            P("fs", None, "tp", None),
        ),
        out_specs=(P("fs", ("sp", "tp"), None), P("fs", None, "tp", "sp")),
        check_vma=False,
    )
```

```python
import jax
import jax.numpy as jnp
from jax import lax
from jax.experimental import pallas as pl
from jax.experimental.pallas import tpu as pltpu
from jax.sharding import PartitionSpec as P

F32 = jnp.float32
BF16 = jnp.bfloat16
SUB = 8
SIN = (3.1415925798055846, -5.16770686616794, 2.5500311935192803, -0.5980441939118888, 0.07721838615680923)
COS = (0.9999999997799038, -4.93480213707883, 4.058709159556464, -1.335212003052184, 0.2349373138245546, -0.024396324364378108)


def poly(coeffs, z):
    total = coeffs[-1]
    for c in coeffs[-2::-1]:
        total = total * z + c
    return total


def dot(a, b, dims=((1,), (0,))):
    return lax.dot_general(a, b, (dims, ((), ())), preferred_element_type=F32)


def iota(shape, dim):
    return lax.broadcasted_iota(jnp.int32, shape, dim)


def cmul(ar, ai, br, bi):
    return ar * br - ai * bi, ar * bi + ai * br


def permutation(rows):
    run = rows // SUB
    r, t = iota((rows, rows), 0), iota((rows, rows), 1)
    return jnp.where((r % SUB) * run + r // SUB == t, 1.0, 0.0).astype(BF16)


def couple(block, state_p, in_r, in_i, dr_ref, di_ref, group, states):
    width = state_p.shape[1]
    span = width // group * states
    rows = slice(block * span, (block + 1) * span)
    tile = jnp.where(iota((group, width), 0) == iota((group, width), 1) % group, 1.0, 0.0).astype(BF16)
    keep = iota((span, width), 0) // states == iota((span, width), 1) // group
    for src, dst in ((in_r, dr_ref), (in_i, di_ref)):
        full = jnp.where(keep, dot(src[rows, :], tile), 0.0).astype(BF16)
        dst[:, rows] = dot(state_p, full, ((1,), (1,)))


def scan_block(lo, span, rate, coef, hr, hi, ar, ai):
    cols = pl.ds(lo, span)
    run = rate.shape[0] // SUB
    reps = span // 128
    decay = jnp.broadcast_to(coef[0:1, cols], (SUB, span))
    turn = jnp.broadcast_to(coef[1:2, cols], (SUB, span))

    def one(j, carry):
        h_r, h_i, a_r, a_i = carry
        at = pl.ds(pl.multiple_of(j * SUB, SUB), SUB)
        r = jnp.concatenate([rate[at, :]] * reps, axis=1)
        u = r * turn
        f = u - jnp.floor(u + 0.5)
        z = f * f
        s = f * poly(SIN, z)
        c = poly(COS, z)
        grow = jnp.exp(r * decay)
        gs = 2.0 * grow * s
        b_r = grow - gs * s
        b_i = gs * c
        p_r, p_i = cmul(b_r - 1.0, b_i, hr[at, cols], hi[at, cols])
        m_r, m_i = cmul(b_r, b_i, h_r, h_i)
        h_r, h_i = m_r + p_r, m_i + p_i
        a_r, a_i = cmul(b_r, b_i, a_r, a_i)
        hr[at, cols] = h_r
        hi[at, cols] = h_i
        ar[at, cols] = a_r
        ai[at, cols] = a_i
        return h_r, h_i, a_r, a_i

    zero = jnp.zeros((SUB, span), F32)
    lax.fori_loop(0, run, one, (zero, zero, zero + 1.0, zero), unroll=2)


def chain_subs(hr, hi, ar, ai, pre, summ):
    rows, flat = hr.shape
    last = rows - SUB
    m_r, m_i = jnp.ones((1, flat), F32), jnp.zeros((1, flat), F32)
    v_r, v_i = jnp.zeros((1, flat), F32), jnp.zeros((1, flat), F32)
    for s in range(SUB):
        row = slice(s, s + 1)
        pre[0, row, :], pre[1, row, :], pre[2, row, :], pre[3, row, :] = m_r, m_i, v_r, v_i
        at = slice(last + s, last + s + 1)
        e_r, e_i = ar[at, :], ai[at, :]
        m_r, m_i = cmul(e_r, e_i, m_r, m_i)
        w_r, w_i = cmul(e_r, e_i, v_r, v_i)
        v_r, v_i = w_r + hr[at, :], w_i + hi[at, :]
    summ[0:1, :], summ[1:2, :], summ[2:3, :], summ[3:4, :] = m_r, m_i, v_r, v_i


def enter_states(place, count, get, opening):
    s_r, s_i = opening[0:1, :], opening[1:2, :]
    e_r, e_i = s_r, s_i
    for j in range(count):
        g = get(j)
        here = place == j
        e_r, e_i = jnp.where(here, s_r, e_r), jnp.where(here, s_i, e_i)
        t_r, t_i = cmul(g[0:1, :], g[1:2, :], s_r, s_i)
        s_r, s_i = t_r + g[2:3, :], t_i + g[3:4, :]
    return e_r, e_i, s_r, s_i


def readout(block, width, state_p, enter, hr, hi, ar, ai, pre, rd_r, rd_i, skip, perm, out, group, states):
    span = width // group * states
    cols = slice(block * span, (block + 1) * span)
    chans = slice(block * width, (block + 1) * width)
    rows = hr.shape[0]
    run = rows // SUB
    e_r, e_i = cmul(pre[0, :, cols], pre[1, :, cols], enter[0][:, cols], enter[1][:, cols])
    e_r, e_i = e_r + pre[2, :, cols], e_i + pre[3, :, cols]
    tile = jnp.where(iota((states, span), 0) == iota((states, span), 1) % states, 1.0, 0.0).astype(BF16)
    keep = iota((width, span), 0) // group == iota((width, span), 1) // states
    g_r = jnp.where(keep, dot(rd_r[chans, :], tile), 0.0).astype(BF16)
    g_i = jnp.where(keep, dot(rd_i[chans, :], tile), 0.0).astype(BF16)

    def fixed(local, a, b, sign):
        a3, b3 = a[:, cols].reshape(run, SUB, span), b[:, cols].reshape(run, SUB, span)
        x, y = (e_r, e_i) if sign < 0 else (e_i, e_r)
        shift = a3 * x[None] + (b3 * y[None] if sign > 0 else -b3 * y[None])
        return (local[:, cols].reshape(run, SUB, span) + shift).reshape(rows, span).astype(BF16)

    total = dot(fixed(hr, ar, ai, -1), g_r, ((1,), (1,))) - dot(fixed(hi, ar, ai, 1), g_i, ((1,), (1,)))
    v = total + skip[:, chans] * state_p[:, chans].astype(F32)
    mix = 0.5 * v * (1.0 + jnp.tanh(0.7978845608 * (v + 0.044715 * (v * v * v))))
    out[:, chans] = dot(perm, mix.astype(BF16), ((0,), (0,))).astype(BF16)


def ssm_prepare(log_step, decay_real, frequency, step_rate, input_real, input_imag, read_real, read_imag, skip_gain, initial_state, rows):
    groups, states = decay_real.shape
    group = skip_gain.shape[1]
    flat = groups * states
    base = jnp.exp(log_step)[:, None]
    coef = jnp.stack([base * decay_real, base * frequency * 0.15915494309189535]).reshape(2, flat)
    modulus = decay_real * decay_real + frequency * frequency
    inv_r, inv_i = (decay_real / modulus)[..., None], (-frequency / modulus)[..., None]
    in_r = (input_real * inv_r - input_imag * inv_i).astype(BF16).reshape(flat, group)
    in_i = (input_real * inv_i + input_imag * inv_r).astype(BF16).reshape(flat, group)
    rd_r = read_real.astype(BF16).reshape(groups * group, states)
    rd_i = read_imag.astype(BF16).reshape(groups * group, states)
    rate = jnp.broadcast_to(step_rate[0].reshape(SUB, rows // SUB).T.reshape(rows, 1), (rows, 128))
    return coef, rate, in_r, in_i, rd_r, rd_i, skip_gain.reshape(1, groups * group), initial_state[0].reshape(2, flat)


MESH = pl.DeviceIdType.MESH
HALO = 16
S, V, I, O, SO, CO = range(6)


def layer_kernel(
    sizes, tokens, gain, w_0, w_1, w_2, w_3, w_4, w_5, rate, coef, in_r, in_i, rd_r, rd_i, skip, taps, opening,
    out, final,
    full, normed, state_p, hr, hi, ar, ai, pre, summ, sums, ext, halo_src, halo_dst, conv_mix, state_mix, partial, got,
    ring_send, ring_recv, sib_send, sib_recv, sum_send, sum_recv, x_send, x_recv, halo_send, halo_recv,
):
    n_sp, n_fs, n_tp, group, states = sizes
    weights = (w_0, w_1, w_2, w_3, w_4, w_5)
    shard = w_0.shape[0]
    rows = tokens.shape[0]
    channels = w_0.shape[1]
    sp, fs, tp = lax.axis_index("sp"), lax.axis_index("fs"), lax.axis_index("tp")
    pairs = n_sp * n_fs // 2
    half = pairs // 2
    mine = sp * n_fs + fs
    parity, chip = mine % 2, mine // 2
    place = jnp.where(chip % 2 == 0, chip // 2, pairs - 1 - chip // 2)

    def pair_at(offset):
        q = (place + offset + pairs) % pairs
        return jnp.where(q < half, q * 2, (pairs - 1 - q) * 2 + 1)

    def device(linear):
        return (linear // n_fs, linear % n_fs, tp)

    neighbours = (device(pair_at(1) * 2 + parity), device(pair_at(-1) * 2 + parity))
    sibling = device(chip * 2 + 1 - parity)
    sp_peers = [((sp + s) % n_sp, fs, tp) for s in range(1, n_sp)]
    tp_peers = [(sp, fs, (tp + s) % n_tp) for s in range(1, n_tp)]

    barrier = pltpu.get_barrier_semaphore()
    greet = list(neighbours) + [sibling] + sp_peers + tp_peers
    for other in greet:
        pl.semaphore_signal(barrier, inc=1, device_id=other, device_id_type=MESH)
    pl.semaphore_wait(barrier, len(greet))

    sent = []

    def send(src, dst, s_sem, r_sem, to):
        copy = pltpu.make_async_remote_copy(src_ref=src, dst_ref=dst, send_sem=s_sem, recv_sem=r_sem, device_id=to, device_id_type=MESH)
        copy.start()
        sent.append(copy)

    def landed(ref, s_sem, r_sem):
        pltpu.make_async_remote_copy(
            src_ref=ref, dst_ref=ref, send_sem=s_sem, recv_sem=r_sem, device_id=sibling, device_id_type=MESH
        ).wait_recv()

    def slot(w, pair, par):
        return full.at[w, pl.ds(pl.multiple_of((pair * 2 + par) * shard, shard), shard), :]

    def rounds(w, way):
        return half if way == w % 2 else pairs - 1 - half

    def source(way, r):
        return pair_at(-1 - r if way == 0 else 1 + r)

    arrived = set()
    shared = set()

    def arrive(w, way, r):
        if (w, way, r) in arrived:
            return
        arrived.add((w, way, r))
        ref = slot(w, source(way, r), parity)
        landed(ref, ring_send.at[w, way, r], ring_recv.at[w, way, r])
        d = 1 + way * half + r
        send(ref, ref, sib_send.at[w, d], sib_recv.at[w, d], sibling)

    def share(w, d, pair):
        if (w, d) not in shared:
            shared.add((w, d))
            landed(slot(w, pair, 1 - parity), sib_send.at[w, d], sib_recv.at[w, d])

    def issue(w, r):
        for way in range(2):
            if r >= rounds(w, way):
                continue
            if r == 0:
                src, at = weights[w], chip
            else:
                arrive(w, way, r - 1)
                at = source(way, r - 1)
                src = slot(w, at, parity)
            send(src, slot(w, at, parity), ring_send.at[w, way, r], ring_recv.at[w, way, r], neighbours[way])
        if r == 0:
            send(weights[w], slot(w, chip, parity), sib_send.at[w, 0], sib_recv.at[w, 0], sibling)
            full[w, pl.ds(pl.multiple_of(mine * shard, shard), shard), :] = weights[w][...]

    def finish(w):
        for r in range(half):
            for way in range(2):
                if r < rounds(w, way):
                    arrive(w, way, r)
        share(w, 0, chip)
        for r in range(half):
            for way in range(2):
                if r < rounds(w, way):
                    share(w, 1 + way * half + r, source(way, r))

    queue = [(S, 0), (V, 0), (S, 1), (I, 0), (S, 2), (O, 0)]
    for r in range(3, half):
        queue += [(S, r), (V, r - 2), (I, r - 2)]
    todo = [(w, r) for r in range(half) for w in (V, I, O) if (w, r) not in queue]
    todo_out = [(w, r) for r in range(half) for w in (SO, CO)]
    at_once = todo[:-2] + todo_out[:1] + todo[-2:-1] + todo_out[1:2] + todo[-1:] + todo_out[2:]
    queue += at_once
    done = [0]

    def advance(count):
        count = max(0, min(count, len(queue) - done[0]))
        for w, r in queue[done[0] : done[0] + count]:
            issue(w, r)
        done[0] += count

    def until(w, r):
        advance(queue.index((w, r)) + 1 - done[0])

    advance(2)

    def norm(j, carry):
        at = pl.ds(pl.multiple_of(j * 32, 32), 32)
        x = tokens[at, :].astype(F32)
        scale = lax.rsqrt(jnp.mean(x * x, axis=-1, keepdims=True) + 1e-06)
        normed[at, :] = (x * scale * gain[...]).astype(BF16)
        return carry

    lax.fori_loop(0, rows // 32, norm, 0)
    perm = permutation(rows)
    until(S, half - 1)
    advance(3)
    finish(S)

    def project(w):
        return dot(normed[...], full[w]).astype(BF16)

    state_p[...] = dot(perm, project(S)).astype(BF16)
    width = min(128, channels)
    span = width // group * states
    blocks = channels // width
    for block in range(blocks):
        couple(block, state_p[:, block * width : (block + 1) * width], in_r, in_i, hr, hi, group, states)
        scan_block(block * span, span, rate, coef, hr, hi, ar, ai)
        advance(1)
    chain_subs(hr, hi, ar, ai, pre, summ)
    until(I, half - 1)
    finish(V)
    value = project(V)
    for s, other in enumerate(sp_peers):
        send(summ, sums.at[sp], sum_send.at[s], sum_recv.at[s], other)
    sums[pl.ds(sp, 1)] = summ[...][None]
    until(O, half - 1)
    finish(I)
    product = (project(I).astype(F32) * value.astype(F32)).astype(BF16)
    halo_src[...] = product[rows - HALO :, :]
    ext[HALO:, :] = product.astype(F32)
    advance(2)
    finish(O)
    outer = project(O)
    send(halo_src, halo_dst, halo_send, halo_recv, ((sp + 1) % n_sp, fs, tp))
    advance(1)
    landed(halo_dst, halo_send, halo_recv)
    ext[:HALO, :] = jnp.where(sp == 0, 0.0, halo_dst[...].astype(F32))
    reach = taps.shape[0] - 1
    filtered = taps[0:1, :] * ext[HALO - reach : HALO - reach + rows, :]
    for tap in range(1, reach + 1):
        at = HALO - reach + tap
        filtered = filtered + taps[tap : tap + 1, :] * ext[at : at + rows, :]
    conv_mix[...] = (outer.astype(F32) * filtered).astype(BF16)
    advance(1)
    for s in range(1, n_sp):
        landed(sums.at[(sp + n_sp - s) % n_sp], sum_send.at[s - 1], sum_recv.at[s - 1])
    e_r, e_i, s_r, s_i = enter_states(sp, n_sp, lambda j: sums[j], opening)
    final[0:1, :] = s_r
    final[1:2, :] = s_i
    for block in range(blocks):
        readout(block, width, state_p, (e_r, e_i), hr, hi, ar, ai, pre, rd_r, rd_i, skip, perm, state_mix, group, states)
        advance(1)
    own_rows = rows // n_tp
    chunks = []

    def compute(pair):
        c = len(chunks)
        at = pl.ds(pl.multiple_of(pair * 2 * shard, 2 * shard), 2 * shard)
        partial[pl.ds(pair, 1)] = (
            dot(state_mix[...], full[SO, at, :], ((1,), (1,))) + dot(conv_mix[...], full[CO, at, :], ((1,), (1,)))
        ).astype(BF16)[None]
        chunks.append(pair)
        if c > 0:
            exchange(c - 1)

    def exchange(c):
        pair = chunks[c]
        for s, other in enumerate(tp_peers):
            theirs = pl.ds(pl.multiple_of(other[2] * own_rows, own_rows), own_rows)
            send(partial.at[pair, theirs, :], got.at[pair, s], x_send.at[c, s], x_recv.at[c, s], other)

    share(SO, 0, chip)
    share(CO, 0, chip)
    compute(chip)
    for r in range(half - 1):
        for w in (SO, CO):
            until(w, r + 1)
        for way in range(2):
            for w in (SO, CO):
                arrive(w, way, r)
            for w in (SO, CO):
                share(w, 1 + way * half + r, source(way, r))
            compute(source(way, r))
    for w in (SO, CO):
        arrive(w, w % 2, half - 1)
    for w in (SO, CO):
        share(w, 1 + (w % 2) * half + half - 1, source(w % 2, half - 1))
    compute(source(0, half - 1))
    exchange(len(chunks) - 1)
    kept = pl.ds(pl.multiple_of(tp * own_rows, own_rows), own_rows)
    for c, pair in enumerate(chunks):
        for s in range(n_tp - 1):
            landed(got.at[pair, s], x_send.at[c, s], x_recv.at[c, s])
    for k in range(pairs):
        total = partial[k, kept, :].astype(F32)
        for s in range(n_tp - 1):
            total = total + got[k, s].astype(F32)
        out[:, k * 2 * shard : (k + 1) * 2 * shard] = total.astype(BF16)
    for copy in sent:
        copy.wait_send()


def body(tokens, norm_gain, w_state_in, w_value, w_outer, w_inner, w_state_out, w_conv_out, log_step, decay_real, frequency, step_rate, input_real, input_imag, read_real, read_imag, skip_gain, conv_taps, initial_state):
    rows, features = tokens.shape[1:]
    groups, states = decay_real.shape
    group = skip_gain.shape[1]
    flat = groups * states
    channels = groups * group
    conv = conv_taps.shape[1]
    n_sp, n_fs, n_tp = (lax.axis_size(a) for a in ("sp", "fs", "tp"))
    shard = w_state_in.shape[0]
    pairs = n_sp * n_fs // 2
    half = pairs // 2
    coef, rate, in_r, in_i, rd_r, rd_i, skip, opening = ssm_prepare(
        log_step, decay_real, frequency, step_rate, input_real, input_imag, read_real, read_imag, skip_gain, initial_state, rows
    )
    vmem = pl.BlockSpec(memory_space=pltpu.VMEM)
    dma = pltpu.SemaphoreType.DMA
    out, final = pl.pallas_call(
        lambda *refs: layer_kernel((n_sp, n_fs, n_tp, group, states), *refs),
        out_shape=(jax.ShapeDtypeStruct((rows // n_tp, features), BF16), jax.ShapeDtypeStruct((2, flat), F32)),
        in_specs=[vmem] * 17,
        out_specs=[vmem] * 2,
        scratch_shapes=[
            pltpu.VMEM((6, n_sp * n_fs * shard, channels), BF16),
            pltpu.VMEM((rows, features), BF16),
            pltpu.VMEM((rows, channels), BF16),
            *[pltpu.VMEM((rows, flat), F32)] * 4,
            pltpu.VMEM((4, SUB, flat), F32),
            pltpu.VMEM((4, flat), F32),
            pltpu.VMEM((n_sp, 4, flat), F32),
            pltpu.VMEM((rows + HALO, conv), F32),
            pltpu.VMEM((HALO, conv), BF16),
            pltpu.VMEM((HALO, conv), BF16),
            pltpu.VMEM((rows, conv), BF16),
            pltpu.VMEM((rows, channels), BF16),
            pltpu.VMEM((pairs, rows, 2 * shard), BF16),
            pltpu.VMEM((pairs, n_tp - 1, rows // n_tp, 2 * shard), BF16),
            dma((6, 2, half)),
            dma((6, 2, half)),
            dma((6, 1 + 2 * half)),
            dma((6, 1 + 2 * half)),
            dma((n_sp - 1,)),
            dma((n_sp - 1,)),
            dma((pairs, n_tp - 1)),
            dma((pairs, n_tp - 1)),
            dma,
            dma,
        ],
        compiler_params=pltpu.CompilerParams(collective_id=0, has_side_effects=True, vmem_limit_bytes=60000 * 1024),
        name="layer",
    )(
        tokens[0], norm_gain[None], w_state_in, w_value, w_inner, w_outer, w_state_out, w_conv_out,
        rate, coef, in_r, in_i, rd_r, rd_i, skip, conv_taps, opening,
    )
    share = states // n_sp
    own = lax.dynamic_slice_in_dim(final.reshape(2, groups, states), lax.axis_index("sp") * share, share, 2)
    return out[None], own[None]


def solution(mesh):
    return jax.shard_map(
        body,
        mesh=mesh,
        in_specs=(
            P("fs", "sp", None),
            P(),
            P(("sp", "fs"), "tp"),
            P(("sp", "fs"), "tp"),
            P(("sp", "fs"), "tp"),
            P(("sp", "fs"), "tp"),
            P(("sp", "fs"), "tp"),
            P(("sp", "fs"), "tp"),
            P("tp"),
            P("tp", None),
            P("tp", None),
            P("fs", "sp"),
            P("tp", None, None),
            P("tp", None, None),
            P("tp", None, None),
            P("tp", None, None),
            P("tp", None),
            P(None, "tp"),
            P("fs", None, "tp", None),
        ),
        out_specs=(P("fs", ("sp", "tp"), None), P("fs", None, "tp", "sp")),
        check_vma=False,
    )
```
